512 devices in a mesh: sp: 32 (over z, core), tp: 16 (over y, x).
Axes of the slice: x: 4, y: 4, z: 16, core: 2. Of those that a mesh axis runs over, the one named last changes fastest.
Arguments:
- queries: bfloat16 [8192, 1024], P('sp', 'tp'), may hold values from -250 to 250
- keys_values: bfloat16 [2, 8192, 256], P(None, 'sp'), may hold values from -8 to 8
- sink_logits: float32 [16], P('tp'), may hold values from 1 to 5
- proj_weight: bfloat16 [1024, 2048], P('tp'), may hold values from -0.75 to 0.75
- residual: bfloat16 [8192, 2048], P('sp', 'tp'), may hold values from -6 to 6
- norm_gain: float32 [2048], replicated, may hold values from 0.1 to 1.9
- routes: int32 [8192, 2], P('sp'), may hold values from 0 to 31, all different within a row; in each aligned block of 256 rows (0 to 255, 256 to 511, ...) at most 32 rows name the same one
- route_weights: float32 [8192, 2], P('sp'), may hold values from 0.2 to 1
- gate_weight: bfloat16 [32, 2048, 2048], P('sp', None, 'tp'), may hold values from -0.125 to 0.125
- up_weight: bfloat16 [32, 2048, 2048], P('sp', None, 'tp'), may hold values from -0.125 to 0.125
- down_weight: bfloat16 [32, 2048, 2048], P('sp', None, 'tp'), may hold values from -0.125 to 0.125
- shared_gate: bfloat16 [2048, 2048], P(None, 'tp'), may hold values from -0.125 to 0.125
- shared_up: bfloat16 [2048, 2048], P(None, 'tp'), may hold values from -0.125 to 0.125
- shared_down: bfloat16 [2048, 2048], P(None, 'tp'), may hold values from -0.125 to 0.125
Outputs:
- output: bfloat16 [8192, 2048], P('sp', 'tp')
The draws below stay inside these ranges and needn't reach their ends.
Inputs may be any that keep to these rules, and one draw needn't show every extreme that they name: `routes`: the 2 experts of a position differ. In each aligned block of 256 positions no expert is named by more than 32 positions, and in some block one expert is named by exactly 32.
All inputs are finite; a program needn't handle non-finite values.
Results may differ from the reference program's by a relative error of at most 0.0067.
Values may be sent and summed in bfloat16 or wider, within the bound.
No kernel may reach another device: no remote copies, remote signals or barrier semaphores. Data moves between devices by JAX's collectives and lax.ppermute only.
A program may use at most 64 MiB of HBM per device.

```python
import math
import jax
import jax.numpy as jnp
import numpy as np
from jax import lax

D = 2048
HEADS = 16
KV_HEADS = 4
HEAD_WIDTH = 64
D_EXP = 2048
WINDOW = 128
TOP_K = 2
TOK_DEV = 256
TOKENS = 8192
EXPERTS = 32
CAP = 32
N_SP = 32


def attention_draws(key):
    query_seed = jax.random.fold_in(key, 101)
    value_seed = jax.random.fold_in(key, 202)
    keys_values = jax.random.normal(value_seed, (2, TOKENS, KV_HEADS * HEAD_WIDTH), jnp.float32)
    queries = jax.random.normal(query_seed, (TOKENS, HEADS * HEAD_WIDTH), jnp.float32)
    keys_values = jnp.clip(keys_values, -8.0, 8.0)
    return (queries, keys_values)


def draw_queries(key, part):
    return attention_draws(key)[0].astype(jnp.bfloat16)


def draw_keys_values(key, part):
    return attention_draws(key)[1].astype(jnp.bfloat16)


def block_scale(stream_key, dims, shards, smallest, largest):
    loudness = 1.0
    for dim, parts in shards:
        heights = jax.random.uniform(jax.random.fold_in(jax.random.fold_in(stream_key, 6), dim), (parts,), jnp.float32, smallest / len(shards), largest / len(shards))
        loudness = loudness * jnp.repeat(jnp.exp(heights), dims[dim] // parts).reshape((-1,) + (1,) * (len(dims) - 1 - dim))
    return loudness


def deal_out(key, own, number, rows, count, top, most, skew):
    sequence = jax.random.permutation(key, count)
    packed, common = shares(count, rows * top, most, skew, True), shares(count, rows * top, most, skew, False)
    places = jnp.arange(count)

    def named(tallies, offset_by):
        used = int((tallies > 0).sum())
        fixed = max(1, used // 4)
        shifted = fixed + (places - fixed + offset_by * (used - fixed)) % max(1, count - fixed)
        return jnp.zeros((count,), jnp.int32).at[sequence[jnp.where(places < fixed, places, shifted)]].set(jnp.asarray(tallies, jnp.int32))

    tallies = jnp.where(number % 4 == 0, named(packed, number // 4), named(common, number - number // 4 - 1))
    mixed = jax.random.permutation(jax.random.fold_in(own, 3), count)
    donor, receiver = mixed[0:count // 2 * 2:2], mixed[1:count // 2 * 2:2]
    slack = jnp.minimum(tallies[donor] - 1, most - tallies[receiver]) // 2
    slack = jnp.where((donor == sequence[0]) | (receiver == sequence[0]) | (tallies[receiver] == 0), 0, jnp.maximum(slack, 0))
    shifted = jax.random.randint(jax.random.fold_in(own, 4), (count // 2,), 0, 1 << 20) % (slack + 1)
    tallies = tallies.at[donor].add(-shifted).at[receiver].add(shifted)
    labels = jnp.searchsorted(jnp.cumsum(tallies), jnp.arange(rows * top), side="right").astype(jnp.int32)
    grid = labels.reshape(top, rows).T
    grid = grid[jax.random.permutation(jax.random.fold_in(own, 1), rows)]
    offset_by = jax.random.randint(jax.random.fold_in(own, 2), (rows, 1), 0, top)
    return jnp.take_along_axis(grid, (jnp.arange(top)[None, :] + offset_by) % top, axis=1)


def shares(number_of, total, limit, skew, full):
    portions = [(1 << 20) // math.isqrt(standing ** skew) + 1 for standing in range(1, number_of + 1)]
    largest = limit if full else min(limit, max(-(-total // number_of), total * portions[0] // sum(portions)))
    least = 1 if total - largest >= number_of - 1 else 0
    given, surplus = [largest] + [least] * (number_of - 1), total - largest - least * (number_of - 1)
    while surplus > 0:
        free = [i for i in range(1, number_of) if given[i] < largest] or [i for i in range(1, number_of) if given[i] < limit]
        mass, remaining = sum([portions[i] for i in free]), surplus
        for i in free:
            extra = min(limit - given[i], max(1, remaining * portions[i] // mass), surplus)
            given[i] = given[i] + extra
            surplus = surplus - extra
    return np.array(given)


def noise(own_key, dims, width, reach, shards=(), held_as=jnp.bfloat16):
    array = width * jax.random.normal(own_key, dims, jnp.float32)
    if shards:
        array = array * block_scale(own_key, dims, shards, -0.22, 0.18)
    return jnp.clip(array, -reach, reach).astype(held_as)


def setup_inputs(seed: int = 0) -> dict:
    key_of = jax.random.split(jax.random.key(seed), 15)
    queries = draw_queries(jax.random.fold_in(key_of[14], 71), 0)
    keys_values = draw_keys_values(jax.random.fold_in(key_of[14], 71), 0)
    sink_logits = jnp.clip(1.0 + 4.0 * jax.random.uniform(key_of[2], (HEADS,), jnp.float32) ** block_scale(key_of[2], (HEADS,), ((0, 16),), -0.2, 0.2), 1.0, 5.0)
    proj_weight = noise(key_of[3], (HEADS * HEAD_WIDTH, D), (HEADS * HEAD_WIDTH // 16) ** -0.5, 0.75, ((0, 16),))
    residual = noise(key_of[4], (TOKENS, D), 1.0, 6.0, ((0, 32), (1, 16)))
    norm_gain = jnp.clip(1.0 + 0.18 * jax.random.normal(key_of[5], (D,), jnp.float32), 0.1, 1.9)
    routes_keys = jax.random.split(jax.random.fold_in(key_of[6], 1), TOKENS // TOK_DEV)
    routes_turns = jax.random.permutation(jax.random.fold_in(key_of[6], 3), TOKENS // TOK_DEV)
    routes = jax.vmap(lambda own, number: deal_out(jax.random.fold_in(key_of[6], 2), own, number, TOK_DEV, EXPERTS, TOP_K, CAP, 1))(routes_keys, routes_turns).reshape((TOKENS, TOP_K))
    route_weights = jnp.clip(0.2 + 0.8 * jax.random.uniform(key_of[7], (TOKENS, TOP_K), jnp.float32) ** block_scale(key_of[7], (TOKENS, TOP_K), ((0, 32),), -0.2, 0.2), 0.2, 1.0)
    gate_weight = noise(key_of[8], (EXPERTS, D, D_EXP), D ** -0.5, 0.125, ((0, 32), (2, 16)))
    up_weight = noise(key_of[9], (EXPERTS, D, D_EXP), D ** -0.5, 0.125, ((0, 32), (2, 16)))
    down_weight = noise(key_of[10], (EXPERTS, D_EXP, D), D_EXP ** -0.5, 0.125, ((0, 32), (2, 16)))
    shared_gate = noise(key_of[11], (D, D_EXP), D ** -0.5, 0.125, ((1, 16),))
    shared_up = noise(key_of[12], (D, D_EXP), D ** -0.5, 0.125, ((1, 16),))
    shared_down = noise(key_of[13], (D_EXP, D), D_EXP ** -0.5, 0.125, ((1, 16),))
    return dict(queries=queries, keys_values=keys_values, sink_logits=sink_logits, proj_weight=proj_weight, residual=residual, norm_gain=norm_gain, routes=routes, route_weights=route_weights, gate_weight=gate_weight, up_weight=up_weight, down_weight=down_weight, shared_gate=shared_gate, shared_up=shared_up, shared_down=shared_down)


norm_eps = 1e-06

def attention_layer(queries, keys_values, sink_logits):
    blocks = TOKENS // WINDOW
    kv_group = HEADS // KV_HEADS
    query_blocks = queries.reshape(blocks, WINDOW, HEADS, HEAD_WIDTH)
    padded = jnp.concatenate([jnp.zeros((2, WINDOW, KV_HEADS * HEAD_WIDTH), keys_values.dtype), keys_values], axis=1)
    padded = padded.reshape(2, TOKENS + WINDOW, KV_HEADS, HEAD_WIDTH)
    earlier = padded[:, :TOKENS].reshape(2, blocks, WINDOW, KV_HEADS, HEAD_WIDTH)
    later = padded[:, WINDOW:].reshape(2, blocks, WINDOW, KV_HEADS, HEAD_WIDTH)
    banded = jnp.concatenate([earlier, later], axis=2)
    query_pos = jnp.arange(WINDOW, dtype=jnp.int32)[:, None]
    key_pos = jnp.arange(2 * WINDOW, dtype=jnp.int32)[None, :]
    distance = WINDOW + query_pos - key_pos
    absolute = jnp.arange(blocks, dtype=jnp.int32)[:, None, None] * WINDOW - WINDOW + key_pos[None]
    allowed = (distance >= 0)[None] & (distance < WINDOW)[None] & (absolute >= 0)

    def one_head(head_number):
        head_queries = lax.dynamic_index_in_dim(query_blocks, head_number, 2, keepdims=False)
        kv_number = head_number // kv_group
        head_keys = lax.dynamic_index_in_dim(banded[0], kv_number, 2, keepdims=False)
        head_values = lax.dynamic_index_in_dim(banded[1], kv_number, 2, keepdims=False)
        score_matrix = jnp.einsum('pvg,pug->pvu', head_queries.astype(jnp.float32), head_keys.astype(jnp.float32)) * HEAD_WIDTH ** (-0.5)
        masked = jnp.where(allowed, score_matrix, -jnp.inf)
        sink_value = sink_logits[head_number].astype(jnp.float32)
        highest = jnp.maximum(lax.optimization_barrier(jnp.max(masked, axis=-1, keepdims=True)), sink_value)
        weights_exp = jnp.exp(masked - highest)
        denominator = lax.optimization_barrier(jnp.sum(weights_exp, axis=-1, keepdims=True)) + jnp.exp(sink_value - highest)
        softmax_weights = (weights_exp / denominator).astype(jnp.bfloat16)
        attended_values = jnp.einsum('ugj,ujs->ugs', softmax_weights.astype(jnp.float32), head_values.astype(jnp.float32))
        return attended_values.astype(jnp.bfloat16)
    per_head = lax.map(one_head, jnp.arange(HEADS, dtype=jnp.int32))
    return jnp.transpose(per_head, (1, 2, 0, 3)).reshape(TOKENS, HEADS * HEAD_WIDTH)

def reference(queries, keys_values, sink_logits, proj_weight, residual, norm_gain, routes, route_weights, gate_weight, up_weight, down_weight, shared_gate, shared_up, shared_down):
    attended_values = attention_layer(queries, keys_values, sink_logits)
    stream_f = jnp.dot(attended_values, proj_weight, preferred_element_type=jnp.float32) + residual.astype(jnp.float32)
    stream = stream_f.astype(jnp.bfloat16)
    stream_wide = stream.astype(jnp.float32)
    row_scale = lax.rsqrt(lax.optimization_barrier(jnp.mean(stream_wide * stream_wide, axis=-1)) + norm_eps)
    gain_col = norm_gain.astype(jnp.float32)[:, None]
    slots = N_SP * CAP
    flat_routes = routes.reshape(-1).astype(jnp.int32)
    assigned = flat_routes.shape[0]
    onehot = (flat_routes[:, None] == jnp.arange(EXPERTS, dtype=jnp.int32)[None, :]).astype(jnp.int32)
    before = jnp.cumsum(onehot, axis=0) - onehot
    slot_rank = lax.optimization_barrier(jnp.sum(before * onehot, axis=1)).astype(jnp.int32)
    token_of = (jnp.arange(assigned, dtype=jnp.int32) // TOP_K).astype(jnp.int32)
    slot_owner = jnp.full((EXPERTS, slots), TOKENS, jnp.int32).at[flat_routes, slot_rank].set(token_of)

    def one_expert(expert):
        owners = slot_owner[expert]
        rows = jnp.take(stream, owners, axis=0, mode='fill', fill_value=0)
        scales = jnp.take(row_scale, owners, axis=0, mode='fill', fill_value=0)
        gate_eff = (gain_col * gate_weight[expert].astype(jnp.float32)).astype(jnp.bfloat16)
        up_eff = (gain_col * up_weight[expert].astype(jnp.float32)).astype(jnp.bfloat16)
        gate_val = scales[:, None] * jnp.dot(rows, gate_eff, preferred_element_type=jnp.float32)
        up_val = scales[:, None] * jnp.dot(rows, up_eff, preferred_element_type=jnp.float32)
        hidden = (jax.nn.silu(gate_val) * up_val).astype(jnp.bfloat16)
        return jnp.dot(hidden, down_weight[expert], preferred_element_type=jnp.float32).astype(jnp.bfloat16)
    expert_out = lax.map(one_expert, jnp.arange(EXPERTS, dtype=jnp.int32))
    picked = expert_out[flat_routes, slot_rank].reshape(TOKENS, TOP_K, D)
    routed = lax.optimization_barrier(jnp.sum(route_weights.astype(jnp.float32)[:, :, None] * picked.astype(jnp.float32), axis=1))
    shared_gate_eff = (gain_col * shared_gate.astype(jnp.float32)).astype(jnp.bfloat16)
    shared_up_eff = (gain_col * shared_up.astype(jnp.float32)).astype(jnp.bfloat16)
    shared_gate_val = row_scale[:, None] * jnp.dot(stream, shared_gate_eff, preferred_element_type=jnp.float32)
    shared_up_val = row_scale[:, None] * jnp.dot(stream, shared_up_eff, preferred_element_type=jnp.float32)
    shared_hidden = (jax.nn.silu(shared_gate_val) * shared_up_val).astype(jnp.bfloat16)
    shared_out = jnp.dot(shared_hidden, shared_down, preferred_element_type=jnp.float32)
    return (stream_wide + shared_out + routed).astype(jnp.bfloat16)
```

```python
import functools

import jax
import jax.numpy as jnp
import numpy as np
from jax import lax
from jax.experimental import pallas as pl
from jax.experimental.pallas import tpu as pltpu
from jax.sharding import PartitionSpec as P

D = 2048
HEADS = 16
KV_HEADS = 4
HEAD_WIDTH = 64
WINDOW = 128
TOK_DEV = 256
N_SP = 32
N_TP = 16
CAP = 32
G = 4
SLOTS = CAP // G
TILE = D // N_TP
EPS = 1e-06
BF = jnp.bfloat16
F32 = jnp.float32


BOTH = ("sp", "tp")


def make_groups(along_r):
    groups = []
    for sp in range(N_SP):
        tiles = np.arange(N_TP).reshape(G, G)
        if (sp % 2 == 0) == along_r:
            tiles = tiles.T
        groups += [[sp * N_TP + int(t) for t in row] for row in tiles]
    return groups


R_GROUPS = make_groups(True)
H_GROUPS = make_groups(False)


def shifted(x, groups, step):
    pairs = [(g[i], g[(i + step) % G]) for g in groups for i in range(G)]
    return lax.ppermute(x, BOTH, pairs)


def swapped(x, groups):
    return lax.all_to_all(x, BOTH, 0, 0, tiled=True, axis_index_groups=groups)


def dot(a, b, dims=(((1,), (0,)), ((), ()))):
    return lax.dot_general(a, b, dims, preferred_element_type=F32)


VM = pl.BlockSpec(memory_space=pltpu.VMEM)
SM = pl.BlockSpec(memory_space=pltpu.SMEM)
PARAMS = pltpu.CompilerParams(vmem_limit_bytes=56 * 1024 * 1024)


def call(kernel, shapes, specs, scratch=()):
    return pl.pallas_call(
        kernel,
        out_shape=shapes,
        in_specs=specs,
        out_specs=jax.tree.map(lambda _: VM, shapes),
        scratch_shapes=list(scratch),
        compiler_params=PARAMS,
    )


def front_kernel(meta, recv, halo, kv, residual, routes_t, stream_out, picked_out, slots_out, att):
    W, HW = WINDOW, HEAD_WIDTH
    row = lax.broadcasted_iota(jnp.int32, (G * W, W), 0) % W
    col = lax.broadcasted_iota(jnp.int32, (G * W, W), 1)
    before = col > row
    first = meta[4] == 0
    for b in range(2):
        for g in range(KV_HEADS):
            lanes = slice(g * HW, (g + 1) * HW)
            if b == 0:
                k_old, v_old = halo[0, :, lanes], halo[1, :, lanes]
            else:
                k_old, v_old = kv[0, :W, lanes], kv[1, :W, lanes]
            k_new, v_new = kv[0, b * W : (b + 1) * W, lanes], kv[1, b * W : (b + 1) * W, lanes]
            heads = [g * (HEADS // KV_HEADS) + i for i in range(HEADS // KV_HEADS)]
            q = jnp.concatenate([recv[h, :W, b * HW : (b + 1) * HW] for h in heads], axis=0)
            sink_rows = [recv[h, 192:193, :].astype(F32) for h in heads]
            sink = jnp.concatenate(
                [
                    jnp.broadcast_to(s[:, 0:1] + s[:, 1:2] + s[:, 2:3], (W, 1))
                    for s in sink_rows
                ],
                axis=0,
            )
            t_dims = (((1,), (1,)), ((), ()))
            s_old = dot(q, k_old, t_dims)
            if b == 0:
                s_old = jnp.where(first, -jnp.inf, s_old)
            score = jnp.where(before, s_old, dot(q, k_new, t_dims)) * HW ** (-0.5)
            top = jnp.maximum(jnp.max(score, axis=1, keepdims=True), sink)
            e = jnp.exp(score - top)
            den = jnp.sum(e, axis=1, keepdims=True) + jnp.exp(sink - top)
            p = e * (1.0 / den)
            p_old = jnp.where(before, p, 0.0).astype(BF)
            p_new = jnp.where(before, 0.0, p).astype(BF)
            a = (dot(p_old, v_old) + dot(p_new, v_new)).astype(BF)
            for i in range(0, len(heads), 2):
                pair = jnp.concatenate([a[i * W : (i + 1) * W], a[(i + 1) * W : (i + 2) * W]], axis=1)
                att[b * W : (b + 1) * W, heads[i] * HW : (heads[i] + 2) * HW] = pair
    weight = recv[:, 128:192, :].reshape(HEADS * HW, TILE)
    stream = (dot(att[...], weight) + residual[...].astype(F32)).astype(BF)
    stream_out[...] = stream
    n = TOK_DEV
    experts = lax.broadcasted_iota(jnp.int32, (N_SP, n), 0)
    hit0 = (experts == routes_t[0:1, :]).astype(F32)
    hit1 = (experts == routes_t[1:2, :]).astype(F32)
    upper = (
        lax.broadcasted_iota(jnp.int32, (n, n), 0) < lax.broadcasted_iota(jnp.int32, (n, n), 1)
    ).astype(F32)
    earlier = dot((hit0 + hit1).astype(BF), upper.astype(BF))
    slot0 = routes_t[0:1, :] * CAP + jnp.sum(earlier * hit0, axis=0, keepdims=True).astype(jnp.int32)
    slot1 = routes_t[1:2, :] * CAP + jnp.sum(earlier * hit1, axis=0, keepdims=True).astype(jnp.int32)
    slots_out[0:1, :] = slot0
    slots_out[1:2, :] = slot1
    step = 256
    for j in range(0, N_SP * CAP, step):
        place = lax.broadcasted_iota(jnp.int32, (step, n), 0) + j
        pick = ((place == slot0) | (place == slot1)).astype(F32).astype(BF)
        picked_out[j : j + step, :] = dot(pick, stream).astype(BF)


def tile_at(meta, s, u):
    r = lax.rem(meta[0] + (G - s), G)
    h = lax.rem(meta[1] + (G - u), G)
    return r * meta[2] + h * meta[3]


def lanes_at(index):
    return pl.ds(pl.multiple_of(index * TILE, TILE), TILE)


def row_scale(x):
    return lax.rsqrt(jnp.sum(x * x, axis=1, keepdims=True) / D + EPS)


def gated(scale, both):
    g = scale * both[:, :TILE]
    u = scale * both[:, TILE:]
    return (g / (1.0 + jnp.exp(-g)) * u).astype(BF)


def shared_kernel(meta, p0, p1, p2, p3, weight, out, x):
    for u, piece in enumerate((p0, p1, p2, p3)):
        for s in range(G):
            x[:, lanes_at(tile_at(meta, s, u))] = piece[s]
    full = x[...]
    out[...] = gated(row_scale(full.astype(F32)), dot(full, weight[...]))


def spread_kernel(meta, arrived, out):
    for t in range(N_TP):
        r = jnp.where(meta[2] == G, t // G, t % G)
        out[t] = arrived[:, r]


def hidden_kernel(rows, weight, shared, out, x):
    for t in range(N_TP):
        x[:, t * TILE : (t + 1) * TILE] = rows[t]
    full = x[...]
    scale = row_scale(full.astype(F32))
    for s in range(G):
        part = gated(scale, dot(full, weight[:, s * 2 * TILE : (s + 1) * 2 * TILE]))
        for k in range(G):
            out[k, :, s * TILE : (s + 1) * TILE] = part
    for k in range(G):
        out[k, :, G * TILE :] = shared[...]


def down_kernel(meta, hidden, down, shared_down, out, x):
    rows = N_SP * SLOTS
    for h in range(G):
        for s in range(G):
            tile = lax.rem(meta[0] + (G - s), G) * meta[2] + h * meta[3]
            x[:, lanes_at(tile)] = hidden[h, :, s * TILE : (s + 1) * TILE]
    result = dot(x[...], down[...]).astype(BF)
    for s in range(G):
        out[lax.rem(meta[0] + (G - s), G), :rows] = result[:, s * TILE : (s + 1) * TILE]
    own = jnp.concatenate([hidden[h, :, G * TILE :] for h in range(G)], axis=1)
    for r in range(G):
        out[r, rows:] = dot(own, shared_down[r]).astype(BF)


def return_kernel(parts, out):
    for r in range(G):
        out[:, r] = parts[r, :N_SP]


def combine_kernel(back, slots, weights_t, stream, parts, out):
    n = TOK_DEV
    total = stream[...].astype(F32)
    for r in range(G):
        total = total + parts[r, N_SP * SLOTS :].astype(F32)
    step = 256
    dims = (((0,), (0,)), ((), ()))
    for j in range(0, N_SP * CAP, step):
        place = lax.broadcasted_iota(jnp.int32, (step, n), 0) + j
        mix = jnp.where(place == slots[0:1, :], weights_t[0:1, :], 0.0) + jnp.where(
            place == slots[1:2, :], weights_t[1:2, :], 0.0
        )
        high = mix.astype(BF)
        low = (mix - high.astype(F32)).astype(BF)
        piece = back[j : j + step, :]
        total = total + dot(high, piece, dims) + dot(low, piece, dims)
    out[...] = total.astype(BF)


def per_device(
    queries,
    keys_values,
    sink_logits,
    proj_weight,
    residual,
    norm_gain,
    routes,
    route_weights,
    gate_weight,
    up_weight,
    down_weight,
    shared_gate,
    shared_up,
    shared_down,
):
    sds = jax.ShapeDtypeStruct
    sp = lax.axis_index("sp")
    tp = lax.axis_index("tp")
    odd = lax.rem(sp, 2)
    high, low = tp // G, lax.rem(tp, G)
    r = jnp.where(odd == 0, high, low)
    h = jnp.where(odd == 0, low, high)
    meta = jnp.stack([r, h, jnp.where(odd == 0, G, 1), jnp.where(odd == 0, 1, G), sp]).astype(
        jnp.int32
    )

    halo = lax.ppermute(
        keys_values[:, TOK_DEV - WINDOW :, :], "sp", [(i, i + 1) for i in range(N_SP - 1)]
    )
    pair = jnp.concatenate([queries[:WINDOW], queries[WINDOW:]], axis=1)
    s0 = lax.reduce_precision(sink_logits, 8, 7)
    s1 = lax.reduce_precision(sink_logits - s0, 8, 7)
    s2 = sink_logits - s0 - s1
    lane = lax.broadcasted_iota(jnp.int32, (16, TILE), 1)
    sink_row = jnp.where(lane == 0, s0, jnp.where(lane == 1, s1, jnp.where(lane == 2, s2, 0.0)))
    fixed = jnp.concatenate([pair, sink_row.astype(BF)], axis=0)
    fixed = jnp.broadcast_to(fixed[None], (N_TP, *fixed.shape))
    columns = proj_weight.reshape(HEAD_WIDTH, N_TP, TILE).transpose(1, 0, 2)
    payload = jnp.concatenate([fixed[:, :WINDOW], columns, fixed[:, WINDOW:]], axis=1)
    recv = lax.all_to_all(payload, "tp", 0, 0, tiled=True)

    gain = norm_gain[:, None]
    gate_eff = (gain * gate_weight[0].astype(F32)).astype(BF)
    up_eff = (gain * up_weight[0].astype(F32)).astype(BF)
    mine = jnp.concatenate([gate_eff, up_eff, down_weight[0]], axis=1)
    pieces = [mine] + [shifted(mine, R_GROUPS, s) for s in range(1, G)]
    gate_up = jnp.concatenate([p[:, : 2 * TILE] for p in pieces], axis=1)
    down = jnp.concatenate([p[:, 2 * TILE :] for p in pieces], axis=1)
    shared_both = jnp.concatenate(
        [
            (gain * shared_gate.astype(F32)).astype(BF),
            (gain * shared_up.astype(F32)).astype(BF),
        ],
        axis=1,
    )
    tiles = shared_down.reshape(G, G, TILE, TILE)
    tiles = jnp.where(odd == 0, tiles, tiles.transpose(1, 0, 2, 3)).reshape(G, G * TILE, TILE)
    recv, tiles = lax.optimization_barrier((recv, tiles))
    shared_rows = swapped(tiles, R_GROUPS)

    stream, picked, slots = call(
        front_kernel,
        (
            sds((TOK_DEV, TILE), BF),
            sds((N_SP * CAP, TILE), BF),
            sds((2, TOK_DEV), jnp.int32),
        ),
        [SM, VM, VM, VM, VM, VM],
        [pltpu.VMEM((TOK_DEV, HEADS * HEAD_WIDTH), BF)],
    )(meta, recv, halo, keys_values, residual, routes.T)

    arrived = lax.all_to_all(picked.reshape(N_SP, CAP, TILE), "sp", 0, 0, tiled=True)

    near = jnp.stack([stream] + [shifted(stream, R_GROUPS, s) for s in range(1, G)])
    blocks = [near] + [shifted(near, H_GROUPS, u) for u in range(1, G)]
    shared_hidden = call(
        shared_kernel,
        sds((TOK_DEV, TILE), BF),
        [SM, VM, VM, VM, VM, VM],
        [pltpu.VMEM((TOK_DEV, D), BF)],
    )(meta, *blocks, shared_both)

    sent = call(
        spread_kernel,
        sds((N_TP, N_SP, SLOTS, TILE), BF),
        [SM, VM],
    )(meta, arrived.reshape(N_SP, G, SLOTS, TILE))
    rows = lax.all_to_all(sent.reshape(N_TP, N_SP * SLOTS, TILE), "tp", 0, 0, tiled=True)

    hidden = call(
        hidden_kernel,
        sds((G, N_SP * SLOTS, (G + 1) * TILE), BF),
        [VM, VM, VM],
        [pltpu.VMEM((N_SP * SLOTS, D), BF)],
    )(rows, gate_up, shared_hidden)
    hidden = swapped(hidden, H_GROUPS)

    parts = call(
        down_kernel,
        sds((G, N_SP * SLOTS + TOK_DEV, TILE), BF),
        [SM, VM, VM, VM],
        [pltpu.VMEM((N_SP * SLOTS, D), BF)],
    )(meta, hidden, down, shared_rows)
    parts = swapped(parts, R_GROUPS)

    outgoing = call(return_kernel, sds((N_SP, G, SLOTS, TILE), BF), [VM])(
        parts.reshape(G, 2 * N_SP, SLOTS, TILE)
    )
    back = lax.all_to_all(outgoing.reshape(N_SP, CAP, TILE), "sp", 0, 0, tiled=True)
    return call(combine_kernel, sds((TOK_DEV, TILE), BF), [VM, VM, VM, VM, VM])(
        back.reshape(N_SP * CAP, TILE), slots, route_weights.T, stream, parts
    )


def solution(mesh):
    placed = (
        P("sp", "tp"),
        P(None, "sp", None),
        P("tp"),
        P("tp", None),
        P("sp", "tp"),
        P(),
        P("sp", None),
        P("sp", None),
        P("sp", None, "tp"),
        P("sp", None, "tp"),
        P("sp", None, "tp"),
        P(None, "tp"),
        P(None, "tp"),
        P(None, "tp"),
    )
    return jax.shard_map(
        per_device, mesh=mesh, in_specs=placed, out_specs=P("sp", "tp"), check_vma=False
    )
```

```python
import jax
import jax.numpy as jnp
import numpy as np
from jax import lax
from jax.experimental import pallas as pl
from jax.experimental.pallas import tpu as pltpu
from jax.sharding import PartitionSpec as P


D = 2048
HEADS = 16
KV_HEADS = 4
HEAD_WIDTH = 64
WINDOW = 128
TOK_DEV = 256
N_SP = 32
N_TP = 16
CAP = 32
G = 4
ROWS = N_SP * CAP // G
OWN = TOK_DEV // G
ALL_ROWS = ROWS + OWN
TILE = D // N_TP
EPS = 1e-06
BF = jnp.bfloat16
F32 = jnp.float32


BOTH = ("sp", "tp")


def make_groups(along_r):
    groups = []
    for sp in range(N_SP):
        tiles = np.arange(N_TP).reshape(G, G)
        if (sp % 2 == 0) == along_r:
            tiles = tiles.T
        groups += [[sp * N_TP + int(t) for t in row] for row in tiles]
    return groups


R_GROUPS = make_groups(True)
H_GROUPS = make_groups(False)


def shifted(x, groups, step):
    pairs = [(g[i], g[(i + step) % G]) for g in groups for i in range(G)]
    return lax.ppermute(x, BOTH, pairs)


def swapped(x, groups):
    return lax.all_to_all(x, BOTH, 0, 0, tiled=True, axis_index_groups=groups)


def dot(a, b, dims=(((1,), (0,)), ((), ()))):
    return lax.dot_general(a, b, dims, preferred_element_type=F32)


VM = pl.BlockSpec(memory_space=pltpu.VMEM)
SM = pl.BlockSpec(memory_space=pltpu.SMEM)
PARAMS = pltpu.CompilerParams(vmem_limit_bytes=16 * 1024 * 1024)


def call(kernel, shapes, specs, scratch=()):
    return pl.pallas_call(
        kernel,
        out_shape=shapes,
        in_specs=specs,
        out_specs=jax.tree.map(lambda _: VM, shapes),
        scratch_shapes=list(scratch),
        compiler_params=PARAMS,
    )


def payload_kernel(sink, queries, proj, out):
    W = WINDOW
    pair = jnp.concatenate([queries[:W], queries[W:]], axis=1)
    logit = jnp.full((16, TILE), sink[0], F32)
    first = logit.astype(BF)
    rest = logit - first.astype(F32)
    second = rest.astype(BF)
    third = (rest - second.astype(F32)).astype(BF)
    lane = lax.broadcasted_iota(jnp.int32, (16, TILE), 1)
    parts = jnp.where(
        lane == 0, first.astype(F32), jnp.where(lane == 1, second.astype(F32), third.astype(F32))
    ).astype(BF)
    for t in range(N_TP):
        out[t, :W] = pair
        out[t, W : W + HEAD_WIDTH] = proj[:, t * TILE : (t + 1) * TILE]
        out[t, W + HEAD_WIDTH :] = parts


def route_kernel(routes_t, slots_out, pick_out):
    n = TOK_DEV
    experts = lax.broadcasted_iota(jnp.int32, (N_SP, n), 0)
    hit0 = (experts == routes_t[0:1, :]).astype(F32)
    hit1 = (experts == routes_t[1:2, :]).astype(F32)
    upper = (
        lax.broadcasted_iota(jnp.int32, (n, n), 0) < lax.broadcasted_iota(jnp.int32, (n, n), 1)
    ).astype(F32)
    earlier = dot((hit0 + hit1).astype(BF), upper.astype(BF))
    slot0 = routes_t[0:1, :] * CAP + jnp.sum(earlier * hit0, axis=0, keepdims=True).astype(jnp.int32)
    slot1 = routes_t[1:2, :] * CAP + jnp.sum(earlier * hit1, axis=0, keepdims=True).astype(jnp.int32)
    slots_out[0:1, :] = slot0
    slots_out[1:2, :] = slot1
    step = 256
    for j in range(0, N_SP * CAP, step):
        place = lax.broadcasted_iota(jnp.int32, (step, n), 0) + j
        pick = (place == slot0) | (place == slot1)
        pick_out[j : j + step, :] = pick.astype(F32).astype(BF)


def front_kernel(meta, recv, halo, kv, residual, pick, stream_out, picked_out, att):
    W, HW = WINDOW, HEAD_WIDTH
    row = lax.broadcasted_iota(jnp.int32, (G * W, W), 0) % W
    col = lax.broadcasted_iota(jnp.int32, (G * W, W), 1)
    before = col > row
    first = meta[4] == 0
    for b in range(2):
        for g in range(KV_HEADS):
            lanes = slice(g * HW, (g + 1) * HW)
            if b == 0:
                k_old, v_old = halo[0, :, lanes], halo[1, :, lanes]
            else:
                k_old, v_old = kv[0, :W, lanes], kv[1, :W, lanes]
            k_new, v_new = kv[0, b * W : (b + 1) * W, lanes], kv[1, b * W : (b + 1) * W, lanes]
            heads = [g * (HEADS // KV_HEADS) + i for i in range(HEADS // KV_HEADS)]
            q = jnp.concatenate([recv[h, :W, b * HW : (b + 1) * HW] for h in heads], axis=0)
            sink_rows = [recv[h, 192:193, :].astype(F32) for h in heads]
            sink = jnp.concatenate(
                [
                    jnp.broadcast_to(s[:, 0:1] + s[:, 1:2] + s[:, 2:3], (W, 1))
                    for s in sink_rows
                ],
                axis=0,
            )
            t_dims = (((1,), (1,)), ((), ()))
            s_old = dot(q, k_old, t_dims)
            if b == 0:
                s_old = jnp.where(first, -jnp.inf, s_old)
            score = jnp.where(before, s_old, dot(q, k_new, t_dims)) * HW ** (-0.5)
            top = jnp.maximum(jnp.max(score, axis=1, keepdims=True), sink)
            e = jnp.exp(score - top)
            den = jnp.sum(e, axis=1, keepdims=True) + jnp.exp(sink - top)
            p = e * (1.0 / den)
            p_old = jnp.where(before, p, 0.0).astype(BF)
            p_new = jnp.where(before, 0.0, p).astype(BF)
            a = (dot(p_old, v_old) + dot(p_new, v_new)).astype(BF)
            for i in range(0, len(heads), 2):
                pair = jnp.concatenate([a[i * W : (i + 1) * W], a[(i + 1) * W : (i + 2) * W]], axis=1)
                att[b * W : (b + 1) * W, heads[i] * HW : (heads[i] + 2) * HW] = pair
    weight = recv[:, 128:192, :].reshape(HEADS * HW, TILE)
    stream = (dot(att[...], weight) + residual[...].astype(F32)).astype(BF)
    stream_out[...] = stream
    picked_out[...] = dot(pick[...], stream).astype(BF)


def lanes_at(index):
    return pl.ds(pl.multiple_of(index * TILE, TILE), TILE)


def row_scale(x):
    return lax.rsqrt(jnp.sum(x * x, axis=1, keepdims=True) / D + EPS)


def gated(scale, both):
    g = scale * both[:, :TILE]
    u = scale * both[:, TILE:]
    return (g / (1.0 + jnp.exp(-g)) * u).astype(BF)


def spread_kernel(meta, arrived, stream, out):
    for t in range(N_TP):
        r = jnp.where(meta[2] == G, t // G, t % G)
        out[t, :ROWS] = arrived[r]
        out[t, ROWS:] = stream[r]


HALF = D // 2


def both_halves(x, top, bottom):
    return dot(x[:, :HALF], top) + dot(x[:, HALF:], bottom)


def hidden_kernel(rows, own, back, top, bottom, ahead, out, x):
    for t in range(N_TP):
        x[:, t * TILE : (t + 1) * TILE] = rows[t]
    for at, part in ((0, slice(0, ROWS)), (3 * TILE, slice(ROWS, ALL_ROWS))):
        full = x[part, :]
        lanes = slice(at, at + 2 * TILE)
        scale = row_scale(full.astype(F32))
        for s in range(G):
            if s == 2:
                sums = both_halves(full, top[:, lanes], bottom[:, lanes])
            else:
                sums = dot(full, (own, back, None, ahead)[s][:, lanes])
            result = gated(scale, sums)
            for k in range(G):
                out[k, part, s * TILE : (s + 1) * TILE] = result


def down_kernel(meta, hidden, own, back, top, bottom, ahead, out, x, w):
    places = [lax.rem(meta[0] + (G - s), G) for s in range(G)]
    for s in range(G):
        for h in range(G):
            tile = places[s] * meta[2] + h * meta[3]
            x[:, lanes_at(tile)] = hidden[h, :, s * TILE : (s + 1) * TILE]
    for at, part in ((2 * TILE, slice(0, ROWS)), (5 * TILE, slice(ROWS, ALL_ROWS))):
        lanes = slice(at, at + TILE)
        for s in range(G):
            cols = slice(s * TILE, (s + 1) * TILE)
            if s == 2:
                w[:HALF, cols] = top[:, lanes]
                w[HALF:, cols] = bottom[:, lanes]
            else:
                w[:, cols] = (own, back, None, ahead)[s][:, lanes]
        result = dot(x[part, :], w[...]).astype(BF)
        for s in range(G):
            out[places[s], part] = result[:, s * TILE : (s + 1) * TILE]


def return_kernel(parts, out):
    for r in range(G):
        out[r] = parts[r, :ROWS]


def combine_kernel(back, slots, weights_t, stream, parts, out):
    n = TOK_DEV
    own = jnp.concatenate([parts[r, ROWS:] for r in range(G)], axis=0)
    total = stream[...].astype(F32) + own.astype(F32)
    step = 256
    dims = (((0,), (0,)), ((), ()))
    for j in range(0, N_SP * CAP, step):
        place = lax.broadcasted_iota(jnp.int32, (step, n), 0) + j
        mix = jnp.where(place == slots[0:1, :], weights_t[0:1, :], 0.0) + jnp.where(
            place == slots[1:2, :], weights_t[1:2, :], 0.0
        )
        high = mix.astype(BF)
        low = (mix - high.astype(F32)).astype(BF)
        piece = back[j : j + step, :]
        total = total + dot(high, piece, dims) + dot(low, piece, dims)
    out[...] = total.astype(BF)


def layer(
    queries,
    keys_values,
    sink_logits,
    proj_weight,
    residual,
    norm_gain,
    routes,
    route_weights,
    gate_weight,
    up_weight,
    down_weight,
    shared_gate,
    shared_up,
    shared_down,
):
    sds = jax.ShapeDtypeStruct
    sp = lax.axis_index("sp")
    tp = lax.axis_index("tp")
    odd = lax.rem(sp, 2)
    high, low = tp // G, lax.rem(tp, G)
    r = jnp.where(odd == 0, high, low)
    h = jnp.where(odd == 0, low, high)
    meta = jnp.stack([r, h, jnp.where(odd == 0, G, 1), jnp.where(odd == 0, 1, G), sp]).astype(
        jnp.int32
    )

    payload = call(
        payload_kernel, sds((N_TP, WINDOW + HEAD_WIDTH + 16, TILE), BF), [SM, VM, VM]
    )(sink_logits, queries, proj_weight)
    recv = lax.all_to_all(payload, "tp", 0, 0, tiled=True)
    halo = lax.ppermute(
        keys_values[:, TOK_DEV - WINDOW :, :], "sp", [(i, i + 1) for i in range(N_SP - 1)]
    )

    gain = norm_gain[:, None]

    def packed(gate, up, down):
        gate_eff = (gain * gate.astype(F32)).astype(BF)
        up_eff = (gain * up.astype(F32)).astype(BF)
        return [gate_eff, up_eff, down]

    own = jnp.concatenate(
        packed(gate_weight[0], up_weight[0], down_weight[0])
        + packed(shared_gate, shared_up, shared_down),
        axis=1,
    )
    behind = shifted(own, R_GROUPS, 1)
    ahead = shifted(own, R_GROUPS, 3)
    top = shifted(behind[:HALF], R_GROUPS, 1)
    bottom = shifted(ahead[HALF:], R_GROUPS, 3)
    weights = (own, behind, top, bottom, ahead)

    slots, pick = call(
        route_kernel,
        (sds((2, TOK_DEV), jnp.int32), sds((N_SP * CAP, TOK_DEV), BF)),
        [VM],
    )(routes.T)
    stream, picked = call(
        front_kernel,
        (sds((TOK_DEV, TILE), BF), sds((N_SP * CAP, TILE), BF)),
        [SM, VM, VM, VM, VM, VM],
        [pltpu.VMEM((TOK_DEV, HEADS * HEAD_WIDTH), BF)],
    )(meta, recv, halo, keys_values, residual, pick)

    arrived = lax.all_to_all(picked.reshape(N_SP, CAP, TILE), "sp", 0, 0, tiled=True)

    sent = call(spread_kernel, sds((N_TP, ALL_ROWS, TILE), BF), [SM, VM, VM])(
        meta, arrived.reshape(G, ROWS, TILE), stream.reshape(G, OWN, TILE)
    )
    rows = lax.all_to_all(sent, "tp", 0, 0, tiled=True)

    hidden = call(
        hidden_kernel,
        sds((G, ALL_ROWS, G * TILE), BF),
        [VM] * 6,
        [pltpu.VMEM((ALL_ROWS, D), BF)],
    )(rows, *weights)
    hidden = swapped(hidden, H_GROUPS)

    parts = call(
        down_kernel,
        sds((G, ALL_ROWS, TILE), BF),
        [SM] + [VM] * 6,
        [pltpu.VMEM((ALL_ROWS, D), BF), pltpu.VMEM((D, G * TILE), BF)],
    )(meta, hidden, *weights)
    parts = swapped(parts, R_GROUPS)

    outgoing = call(return_kernel, sds((G, ROWS, TILE), BF), [VM])(parts)
    back = lax.all_to_all(outgoing.reshape(N_SP, CAP, TILE), "sp", 0, 0, tiled=True)
    return call(combine_kernel, sds((TOK_DEV, TILE), BF), [VM, VM, VM, VM, VM])(
        back.reshape(N_SP * CAP, TILE), slots, route_weights.T, stream, parts
    )


def solution(mesh):
    placed = (
        P("sp", "tp"),
        P(None, "sp", None),
        P("tp"),
        P("tp", None),
        P("sp", "tp"),
        P(),
        P("sp", None),
        P("sp", None),
        P("sp", None, "tp"),
        P("sp", None, "tp"),
        P("sp", None, "tp"),
        P(None, "tp"),
        P(None, "tp"),
        P(None, "tp"),
    )
    return jax.shard_map(
        layer, mesh=mesh, in_specs=placed, out_specs=P("sp", "tp"), check_vma=False
    )
```

```python
import jax
import jax.numpy as jnp
import numpy as np
from jax import lax
from jax.experimental import pallas as pl
from jax.experimental.pallas import tpu as pltpu
from jax.sharding import PartitionSpec as P


D = 2048
HEADS = 16
KV_HEADS = 4
HEAD_WIDTH = 64
WINDOW = 128
TOK_DEV = 256
N_SP = 32
N_TP = 16
CAP = 32
G = 4
ROWS = N_SP * CAP // G
OWN = TOK_DEV // G
ALL_ROWS = ROWS + OWN
TILE = D // N_TP
EPS = 1e-06
HALF = D // 2
BF = jnp.bfloat16
F32 = jnp.float32


BOTH = ("sp", "tp")


def make_groups(along_r):
    groups = []
    for sp in range(N_SP):
        tiles = np.arange(N_TP).reshape(G, G)
        if (sp % 2 == 0) == along_r:
            tiles = tiles.T
        groups += [[sp * N_TP + int(t) for t in row] for row in tiles]
    return groups


R_GROUPS = make_groups(True)
H_GROUPS = make_groups(False)


def shifted(x, groups, step):
    pairs = [(g[i], g[(i + step) % G]) for g in groups for i in range(G)]
    return lax.ppermute(x, BOTH, pairs)


def swapped(x, groups):
    return lax.all_to_all(x, BOTH, 0, 0, tiled=True, axis_index_groups=groups)


def dot(a, b, dims=(((1,), (0,)), ((), ()))):
    return lax.dot_general(a, b, dims, preferred_element_type=F32)


VM = pl.BlockSpec(memory_space=pltpu.VMEM)
SM = pl.BlockSpec(memory_space=pltpu.SMEM)
HB = pl.BlockSpec(memory_space=pltpu.HBM)
PARAMS = pltpu.CompilerParams(vmem_limit_bytes=24 * 1024 * 1024)


def call(kernel, shapes, specs, scratch=(), outs=None):
    return pl.pallas_call(
        kernel,
        out_shape=shapes,
        in_specs=specs,
        out_specs=outs or jax.tree.map(lambda _: VM, shapes),
        scratch_shapes=list(scratch),
        compiler_params=PARAMS,
    )


def payload_kernel(sink, queries_t, proj_at, out, proj, sem):
    W = WINDOW
    copy = pltpu.make_async_copy(proj_at, proj, sem)
    copy.start()
    pair = jnp.concatenate([queries_t[:, :W], queries_t[:, W:]], axis=0).T
    logit = jnp.full((16, TILE), sink[0], F32)
    first = logit.astype(BF)
    rest = logit - first.astype(F32)
    second = rest.astype(BF)
    third = (rest - second.astype(F32)).astype(BF)
    lane = lax.broadcasted_iota(jnp.int32, (16, TILE), 1)
    parts = jnp.where(
        lane == 0, first.astype(F32), jnp.where(lane == 1, second.astype(F32), third.astype(F32))
    ).astype(BF)
    copy.wait()
    for t in range(N_TP):
        out[t, :W] = pair
        out[t, W : W + HEAD_WIDTH] = proj[:, t * TILE : (t + 1) * TILE]
        out[t, W + HEAD_WIDTH :] = parts


def prep_kernel(
    gain, gate, up, down, s_gate, s_up, s_down, top, bottom, raw, scaled, sems
):
    def lanes(j):
        return slice(j * TILE, (j + 1) * TILE)

    halves = ((top, slice(0, HALF)), (bottom, slice(HALF, D)))

    scale_from = ((0, gate), (1, up), (3, s_gate), (4, s_up))
    loads = [pltpu.make_async_copy(ref, raw.at[i], sems.at[i]) for i, (_, ref) in enumerate(scale_from)]
    moves = [
        pltpu.make_async_copy(ref.at[rows], out.at[:, lanes(j)], sems.at[4 + 2 * i + k])
        for i, (j, ref) in enumerate(((2, down), (5, s_down)))
        for k, (out, rows) in enumerate(halves)
    ]
    for copy in loads + moves:
        copy.start()
    columns = [
        jnp.broadcast_to(gain[k : k + 1, :], (TILE, TILE)).T for k in range(D // TILE)
    ]
    stores = []
    for i, (j, _) in enumerate(scale_from):
        loads[i].wait()
        for k in range(D // TILE):
            rows = slice(k * TILE, (k + 1) * TILE)
            scaled[i, rows, :] = (columns[k] * raw[i, rows, :].astype(F32)).astype(BF)
        for k, (out, rows) in enumerate(halves):
            target = out.at[:, lanes(j)]
            stores.append(
                pltpu.make_async_copy(scaled.at[i, rows], target, sems.at[8 + 2 * i + k])
            )
            stores[-1].start()
    for copy in moves + stores:
        copy.wait()


def route_mask(routes_t, slots_out, pick):
    n = TOK_DEV
    experts = lax.broadcasted_iota(jnp.int32, (N_SP, n), 0)
    hit0 = (experts == routes_t[0:1, :]).astype(F32)
    hit1 = (experts == routes_t[1:2, :]).astype(F32)
    upper = (
        lax.broadcasted_iota(jnp.int32, (n, n), 0) < lax.broadcasted_iota(jnp.int32, (n, n), 1)
    ).astype(F32)
    earlier = dot((hit0 + hit1).astype(BF), upper.astype(BF))
    slot0 = routes_t[0:1, :] * CAP + jnp.sum(earlier * hit0, axis=0, keepdims=True).astype(jnp.int32)
    slot1 = routes_t[1:2, :] * CAP + jnp.sum(earlier * hit1, axis=0, keepdims=True).astype(jnp.int32)
    slots_out[0:1, :] = slot0
    slots_out[1:2, :] = slot1
    step = 256
    for j in range(0, N_SP * CAP, step):
        place = lax.broadcasted_iota(jnp.int32, (step, n), 0) + j
        hit = (place == slot0) | (place == slot1)
        pick[j : j + step, :] = hit.astype(F32).astype(BF)


def front_kernel(
    meta, routes_t, recv_at, halo_at, kv_at, residual_at, stream_out, picked_at, slots_out,
    recv, halo, kv, residual, pick, att, picked, sems,
):
    W, HW = WINDOW, HEAD_WIDTH
    pairs = ((kv_at, kv), (halo_at, halo), (recv_at, recv), (residual_at, residual))
    copies = [pltpu.make_async_copy(a, b, sems.at[i]) for i, (a, b) in enumerate(pairs)]
    for copy in copies:
        copy.start()
    route_mask(routes_t, slots_out, pick)
    for copy in copies[:3]:
        copy.wait()
    row = lax.broadcasted_iota(jnp.int32, (G * W, W), 0) % W
    col = lax.broadcasted_iota(jnp.int32, (G * W, W), 1)
    before = col > row
    left = lax.broadcasted_iota(jnp.int32, (W, W), 1) < HW
    first = meta[4] == 0
    nothing = jnp.zeros((W, HW), BF)
    t_dims = (((1,), (1,)), ((), ()))
    for g in range(KV_HEADS):
        lanes = slice(g * HW, (g + 1) * HW)
        blocks = [halo[:, :, lanes], kv[:, :W, lanes], kv[:, W:, lanes]]
        values = [jnp.concatenate([v[1], v[1]], axis=1) for v in blocks]
        q = recv[g * G : (g + 1) * G, :W, :].reshape(G * W, TILE) * BF(HW ** (-0.5))
        sink = jnp.concatenate(
            [
                jnp.broadcast_to(jnp.sum(recv[g * G + i, W + HW : W + HW + 1, :3].astype(F32), axis=1, keepdims=True), (W, 1))
                for i in range(G)
            ],
            axis=0,
        )
        for b in range(2):
            keys = [
                jnp.concatenate([k[0], nothing] if b == 0 else [nothing, k[0]], axis=1)
                for k in blocks[b : b + 2]
            ]
            s_old = dot(q, keys[0], t_dims)
            if b == 0:
                s_old = jnp.where(first, -jnp.inf, s_old)
            score = jnp.where(before, s_old, dot(q, keys[1], t_dims))
            top = jnp.maximum(jnp.max(score, axis=1, keepdims=True), sink)
            e = jnp.exp(score - top)
            den = jnp.sum(e, axis=1, keepdims=True) + jnp.exp(sink - top)
            p = e * (1.0 / den)
            p_old = jnp.where(before, p, 0.0).astype(BF)
            p_new = jnp.where(before, 0.0, p).astype(BF)
            a = (dot(p_old, values[b]) + dot(p_new, values[b + 1])).astype(F32)
            for i in range(0, G, 2):
                both = jnp.where(left, a[i * W : (i + 1) * W], a[(i + 1) * W : (i + 2) * W])
                h = g * G + i
                att[b * W : (b + 1) * W, h * HW : (h + 2) * HW] = both.astype(BF)
    copies[3].wait()
    weight = recv[:, W : W + HW, :].reshape(HEADS * HW, TILE)
    stream = (dot(att[...], weight) + residual[...].astype(F32)).astype(BF)
    stream_out[...] = stream
    sends = []
    step = 512
    for i in range(N_SP * CAP // step):
        rows = slice(i * step, (i + 1) * step)
        picked[rows, :] = dot(pick[rows, :], stream).astype(BF)
        sends.append(pltpu.make_async_copy(picked.at[rows], picked_at.at[rows], sems.at[4 + i]))
        sends[-1].start()
    for send in sends:
        send.wait()


def lanes_at(index):
    return pl.ds(pl.multiple_of(index * TILE, TILE), TILE)


def row_scale(x):
    return lax.rsqrt(jnp.sum(x * x, axis=1, keepdims=True) / D + EPS)


def gated(scale, both):
    g = scale * both[:, :TILE]
    u = scale * both[:, TILE:]
    return (g / (1.0 + jnp.exp(-g)) * u).astype(BF)


def spread_kernel(meta, arrived, stream, out):
    for t in range(N_TP):
        r = jnp.where(meta[2] == G, t // G, t % G)
        out[t, :ROWS] = arrived[r]
        out[t, ROWS:] = stream[r]


def piece_copies(refs, lanes, target, sems):
    high, low = slice(0, HALF), slice(HALF, D)
    parts = [(i // 2, ref, low if i % 2 else high) for i, ref in enumerate(refs)]
    return [
        (s, pltpu.make_async_copy(ref.at[:, lanes], target(s, rows), sems.at[i]))
        for i, (s, ref, rows) in enumerate(parts)
    ]


def hidden_kernel(rows, *args):
    refs, (out, x, w, sems) = args[: 2 * G], args[2 * G :]
    sets = [
        piece_copies(
            refs,
            slice(at, at + 2 * TILE),
            lambda s, r, j=j: w.at[j, s, r],
            sems.at[j],
        )
        for j, at in ((0, 0), (1, 3 * TILE))
    ]
    for copies in sets:
        for _, copy in copies:
            copy.start()
    for t in range(N_TP):
        x[:, t * TILE : (t + 1) * TILE] = rows[t]
    for j, part in ((0, slice(0, ROWS)), (1, slice(ROWS, ALL_ROWS))):
        full = x[part, :]
        scale = row_scale(full.astype(F32))
        for s in range(G):
            for step, copy in sets[j]:
                if step == s:
                    copy.wait()
            result = gated(scale, dot(full, w[j, s]))
            for k in range(G):
                out[k, part, s * TILE : (s + 1) * TILE] = result


def down_kernel(meta, hidden, *args):
    refs, (out, x, w, sems) = args[: 2 * G], args[2 * G :]
    sets = [
        piece_copies(
            refs,
            slice(at, at + TILE),
            lambda s, r, j=j: w.at[j, r, pl.ds(s * TILE, TILE)],
            sems.at[j],
        )
        for j, at in ((0, 2 * TILE), (1, 5 * TILE))
    ]
    for copies in sets:
        for _, copy in copies:
            copy.start()
    places = [lax.rem(meta[0] + (G - s), G) for s in range(G)]
    for s in range(G):
        for h in range(G):
            tile = places[s] * meta[2] + h * meta[3]
            x[:, lanes_at(tile)] = hidden[h, :, s * TILE : (s + 1) * TILE]
    for j, part in ((0, slice(0, ROWS)), (1, slice(ROWS, ALL_ROWS))):
        for _, copy in sets[j]:
            copy.wait()
        result = dot(x[part, :], w[j]).astype(BF)
        for s in range(G):
            out[places[s], part] = result[:, s * TILE : (s + 1) * TILE]


def return_kernel(parts, out):
    for r in range(G):
        out[r] = parts[r, :ROWS]


def combine_kernel(back, slots, weights_t, stream, parts, out):
    n = TOK_DEV
    own = jnp.concatenate([parts[r, ROWS:] for r in range(G)], axis=0)
    total = stream[...].astype(F32) + own.astype(F32)
    step = 256
    dims = (((0,), (0,)), ((), ()))
    for j in range(0, N_SP * CAP, step):
        place = lax.broadcasted_iota(jnp.int32, (step, n), 0) + j
        mix = jnp.where(place == slots[0:1, :], weights_t[0:1, :], 0.0) + jnp.where(
            place == slots[1:2, :], weights_t[1:2, :], 0.0
        )
        high = mix.astype(BF)
        low = (mix - high.astype(F32)).astype(BF)
        piece = back[j : j + step, :]
        total = total + dot(high, piece, dims) + dot(low, piece, dims)
    out[...] = total.astype(BF)


def layer(
    queries,
    keys_values,
    sink_logits,
    proj_weight,
    residual,
    norm_gain,
    routes,
    route_weights,
    gate_weight,
    up_weight,
    down_weight,
    shared_gate,
    shared_up,
    shared_down,
):
    sds = jax.ShapeDtypeStruct

    def kept(x):
        return pltpu.with_memory_space_constraint(x, pltpu.HBM)

    sp = lax.axis_index("sp")
    tp = lax.axis_index("tp")
    odd = lax.rem(sp, 2)
    high, low = tp // G, lax.rem(tp, G)
    r = jnp.where(odd == 0, high, low)
    h = jnp.where(odd == 0, low, high)
    meta = jnp.stack([r, h, jnp.where(odd == 0, G, 1), jnp.where(odd == 0, 1, G), sp]).astype(
        jnp.int32
    )

    payload = call(
        payload_kernel,
        sds((N_TP, WINDOW + HEAD_WIDTH + 16, TILE), BF),
        [SM, VM, HB],
        [pltpu.VMEM(proj_weight.shape, BF), pltpu.SemaphoreType.DMA],
    )(sink_logits, queries.T, kept(proj_weight))
    recv = lax.all_to_all(payload, "tp", 0, 0, tiled=True)
    halo = lax.ppermute(
        keys_values[:, TOK_DEV - WINDOW :, :], "sp", [(i, i + 1) for i in range(N_SP - 1)]
    )

    half = sds((HALF, 6 * TILE), BF)
    own_top, own_bottom = call(
        prep_kernel,
        (half, half),
        [VM] + [HB] * 6,
        [
            pltpu.VMEM((4, D, TILE), BF),
            pltpu.VMEM((4, D, TILE), BF),
            pltpu.SemaphoreType.DMA((16,)),
        ],
        outs=(HB, HB),
    )(
        norm_gain.reshape(N_TP, TILE),
        kept(gate_weight[0]),
        kept(up_weight[0]),
        kept(down_weight[0]),
        kept(shared_gate),
        kept(shared_up),
        kept(shared_down),
    )
    behind_top = shifted(own_top, R_GROUPS, 1)
    ahead_bottom = shifted(own_bottom, R_GROUPS, 3)
    behind_bottom = shifted(own_bottom, R_GROUPS, 1)
    ahead_top = shifted(own_top, R_GROUPS, 3)
    top = shifted(behind_top, R_GROUPS, 1)
    bottom = shifted(ahead_bottom, R_GROUPS, 3)
    weights = (
        own_top, own_bottom, behind_top, behind_bottom, top, bottom, ahead_top, ahead_bottom
    )

    rows = N_SP * CAP
    stream, picked, slots = call(
        front_kernel,
        (sds((TOK_DEV, TILE), BF), sds((rows, TILE), BF), sds((2, TOK_DEV), jnp.int32)),
        [SM, VM, HB, HB, HB, HB],
        [
            pltpu.VMEM(recv.shape, BF),
            pltpu.VMEM(halo.shape, BF),
            pltpu.VMEM(keys_values.shape, BF),
            pltpu.VMEM(residual.shape, BF),
            pltpu.VMEM((rows, TOK_DEV), BF),
            pltpu.VMEM((TOK_DEV, HEADS * HEAD_WIDTH), BF),
            pltpu.VMEM((rows, TILE), BF),
            pltpu.SemaphoreType.DMA((6,)),
        ],
        outs=(VM, HB, VM),
    )(meta, routes.T, kept(recv), kept(halo), kept(keys_values), kept(residual))

    arrived = lax.all_to_all(picked.reshape(N_SP, CAP, TILE), "sp", 0, 0, tiled=True)

    sent = call(spread_kernel, sds((N_TP, ALL_ROWS, TILE), BF), [SM, VM, VM])(
        meta, arrived.reshape(G, ROWS, TILE), stream.reshape(G, OWN, TILE)
    )
    rows = lax.all_to_all(sent, "tp", 0, 0, tiled=True)

    hidden = call(
        hidden_kernel,
        sds((G, ALL_ROWS, G * TILE), BF),
        [VM] + [HB] * (2 * G),
        [
            pltpu.VMEM((ALL_ROWS, D), BF),
            pltpu.VMEM((2, G, D, 2 * TILE), BF),
            pltpu.SemaphoreType.DMA((2, 2 * G)),
        ],
    )(rows, *weights)
    hidden = swapped(hidden, H_GROUPS)

    parts = call(
        down_kernel,
        sds((G, ALL_ROWS, TILE), BF),
        [SM, VM] + [HB] * (2 * G),
        [
            pltpu.VMEM((ALL_ROWS, D), BF),
            pltpu.VMEM((2, D, G * TILE), BF),
            pltpu.SemaphoreType.DMA((2, 2 * G)),
        ],
    )(meta, hidden, *weights)
    parts = swapped(parts, R_GROUPS)

    outgoing = call(return_kernel, sds((G, ROWS, TILE), BF), [VM])(parts)
    back = lax.all_to_all(outgoing.reshape(N_SP, CAP, TILE), "sp", 0, 0, tiled=True)
    return call(combine_kernel, sds((TOK_DEV, TILE), BF), [VM, VM, VM, VM, VM])(
        back.reshape(N_SP * CAP, TILE), slots, route_weights.T, stream, parts
    )


def solution(mesh):
    placed = (
        P("sp", "tp"),
        P(None, "sp", None),
        P("tp"),
        P("tp", None),
        P("sp", "tp"),
        P(),
        P("sp", None),
        P("sp", None),
        P("sp", None, "tp"),
        P("sp", None, "tp"),
        P("sp", None, "tp"),
        P(None, "tp"),
        P(None, "tp"),
        P(None, "tp"),
    )
    return jax.shard_map(
        layer, mesh=mesh, in_specs=placed, out_specs=P("sp", "tp"), check_vma=False
    )
```

```python
import jax
import jax.numpy as jnp
import numpy as np
from jax import lax
from jax.experimental import pallas as pl
from jax.experimental.pallas import tpu as pltpu
from jax.sharding import PartitionSpec as P


D = 2048
HEADS = 16
KV_HEADS = 4
HEAD_WIDTH = 64
WINDOW = 128
TOK_DEV = 256
N_SP = 32
N_TP = 16
CAP = 32
G = 4
ROWS = N_SP * CAP // G
OWN = TOK_DEV // G
ALL_ROWS = ROWS + OWN
TILE = D // N_TP
EPS = 1e-06
HALF = D // 2
AHEAD = 8
BF = jnp.bfloat16
F32 = jnp.float32


BOTH = ("sp", "tp")


def make_groups(along_r):
    groups = []
    for sp in range(N_SP):
        tiles = np.arange(N_TP).reshape(G, G)
        if (sp % 2 == 0) == along_r:
            tiles = tiles.T
        groups += [[sp * N_TP + int(t) for t in row] for row in tiles]
    return groups


R_GROUPS = make_groups(True)
H_GROUPS = make_groups(False)


def shifted(x, groups, step):
    pairs = [(g[i], g[(i + step) % G]) for g in groups for i in range(G)]
    return lax.ppermute(x, BOTH, pairs)


def swapped(x, groups):
    return lax.all_to_all(x, BOTH, 0, 0, tiled=True, axis_index_groups=groups)


def dot(a, b, dims=(((1,), (0,)), ((), ()))):
    return lax.dot_general(a, b, dims, preferred_element_type=F32)


VM = pl.BlockSpec(memory_space=pltpu.VMEM)
SM = pl.BlockSpec(memory_space=pltpu.SMEM)
HB = pl.BlockSpec(memory_space=pltpu.HBM)
PARAMS = pltpu.CompilerParams(vmem_limit_bytes=24 * 1024 * 1024)


def call(kernel, shapes, specs, scratch=(), outs=None):
    return pl.pallas_call(
        kernel,
        out_shape=shapes,
        in_specs=specs,
        out_specs=outs or jax.tree.map(lambda _: VM, shapes),
        scratch_shapes=list(scratch),
        compiler_params=PARAMS,
    )


def payload_kernel(sink, queries_at, proj_at, out, queries_t, proj, sems):
    W = WINDOW
    copy = pltpu.make_async_copy(proj_at, proj, sems.at[0])
    copy.start()
    first_copy = pltpu.make_async_copy(queries_at, queries_t, sems.at[1])
    first_copy.start()
    first_copy.wait()
    pair = jnp.concatenate([queries_t[:, :W], queries_t[:, W:]], axis=0).T
    logit = jnp.full((16, TILE), sink[0], F32)
    first = logit.astype(BF)
    rest = logit - first.astype(F32)
    second = rest.astype(BF)
    third = (rest - second.astype(F32)).astype(BF)
    lane = lax.broadcasted_iota(jnp.int32, (16, TILE), 1)
    parts = jnp.where(
        lane == 0, first.astype(F32), jnp.where(lane == 1, second.astype(F32), third.astype(F32))
    ).astype(BF)
    copy.wait()
    for t in range(N_TP):
        out[t, :W] = pair
        out[t, W : W + HEAD_WIDTH] = proj[:, t * TILE : (t + 1) * TILE]
        out[t, W + HEAD_WIDTH :] = parts


def prep_kernel(
    gain, gate, up, down, s_gate, s_up, s_down, top, bottom, raw, scaled, sems
):
    def lanes(j):
        return slice(j * TILE, (j + 1) * TILE)

    halves = ((top, slice(0, HALF)), (bottom, slice(HALF, D)))

    scale_from = ((0, gate), (1, up), (3, s_gate), (4, s_up))
    loads = [pltpu.make_async_copy(ref, raw.at[i], sems.at[i]) for i, (_, ref) in enumerate(scale_from)]
    moves = [
        pltpu.make_async_copy(ref.at[rows], out.at[:, lanes(j)], sems.at[4 + 2 * i + k])
        for i, (j, ref) in enumerate(((2, down), (5, s_down)))
        for k, (out, rows) in enumerate(halves)
    ]
    for copy in loads + moves:
        copy.start()
    columns = [
        jnp.broadcast_to(gain[k : k + 1, :], (TILE, TILE)).T for k in range(D // TILE)
    ]
    stores = []
    for i, (j, _) in enumerate(scale_from):
        loads[i].wait()
        for k in range(D // TILE):
            rows = slice(k * TILE, (k + 1) * TILE)
            scaled[i, rows, :] = (columns[k] * raw[i, rows, :].astype(F32)).astype(BF)
        for k, (out, rows) in enumerate(halves):
            target = out.at[:, lanes(j)]
            stores.append(
                pltpu.make_async_copy(scaled.at[i, rows], target, sems.at[8 + 2 * i + k])
            )
            stores[-1].start()
    for copy in moves + stores:
        copy.wait()


def route_mask(routes_t, slots_out, pick):
    n = TOK_DEV
    experts = lax.broadcasted_iota(jnp.int32, (N_SP, n), 0)
    hit0 = (experts == routes_t[0:1, :]).astype(F32)
    hit1 = (experts == routes_t[1:2, :]).astype(F32)
    upper = (
        lax.broadcasted_iota(jnp.int32, (n, n), 0) < lax.broadcasted_iota(jnp.int32, (n, n), 1)
    ).astype(F32)
    earlier = dot((hit0 + hit1).astype(BF), upper.astype(BF))
    slot0 = routes_t[0:1, :] * CAP + jnp.sum(earlier * hit0, axis=0, keepdims=True).astype(jnp.int32)
    slot1 = routes_t[1:2, :] * CAP + jnp.sum(earlier * hit1, axis=0, keepdims=True).astype(jnp.int32)
    slots_out[0:1, :] = slot0
    slots_out[1:2, :] = slot1
    step = 256
    for j in range(0, N_SP * CAP, step):
        place = lax.broadcasted_iota(jnp.int32, (step, n), 0) + j
        hit = (place == slot0) | (place == slot1)
        pick[j : j + step, :] = hit.astype(F32).astype(BF)


def front_kernel(
    meta, routes_t, recv_at, halo, kv_at, residual_at, stream_out, picked_out, slots_out,
    recv, kv, residual, pick, att, sems,
):
    W, HW = WINDOW, HEAD_WIDTH
    pairs = [(kv_at, kv), (residual_at, residual)]
    for g in range(KV_HEADS):
        heads = slice(g * G, (g + 1) * G)
        pairs.append((recv_at.at[heads], recv.at[heads]))
    copies = [pltpu.make_async_copy(a, b, sems.at[i]) for i, (a, b) in enumerate(pairs)]
    for copy in copies:
        copy.start()
    route_mask(routes_t, slots_out, pick)
    copies[0].wait()
    row = lax.broadcasted_iota(jnp.int32, (G * W, W), 0) % W
    col = lax.broadcasted_iota(jnp.int32, (G * W, W), 1)
    before = col > row
    left = lax.broadcasted_iota(jnp.int32, (W, W), 1) < HW
    first = meta[4] == 0
    nothing = jnp.zeros((W, HW), BF)
    t_dims = (((1,), (1,)), ((), ()))
    for g in range(KV_HEADS):
        lanes = slice(g * HW, (g + 1) * HW)
        blocks = [halo[:, :, lanes], kv[:, :W, lanes], kv[:, W:, lanes]]
        values = [jnp.concatenate([v[1], v[1]], axis=1) for v in blocks]
        copies[2 + g].wait()
        q = recv[g * G : (g + 1) * G, :W, :].reshape(G * W, TILE) * BF(HW ** (-0.5))
        sink = jnp.concatenate(
            [
                jnp.broadcast_to(jnp.sum(recv[g * G + i, W + HW : W + HW + 1, :3].astype(F32), axis=1, keepdims=True), (W, 1))
                for i in range(G)
            ],
            axis=0,
        )
        for b in range(2):
            keys = [
                jnp.concatenate([k[0], nothing] if b == 0 else [nothing, k[0]], axis=1)
                for k in blocks[b : b + 2]
            ]
            s_old = dot(q, keys[0], t_dims)
            if b == 0:
                s_old = jnp.where(first, -jnp.inf, s_old)
            score = jnp.where(before, s_old, dot(q, keys[1], t_dims))
            top = jnp.maximum(jnp.max(score, axis=1, keepdims=True), sink)
            e = jnp.exp(score - top)
            den = jnp.sum(e, axis=1, keepdims=True) + jnp.exp(sink - top)
            p = e * (1.0 / den)
            p_old = jnp.where(before, p, 0.0).astype(BF)
            p_new = jnp.where(before, 0.0, p).astype(BF)
            a = (dot(p_old, values[b]) + dot(p_new, values[b + 1])).astype(F32)
            for i in range(0, G, 2):
                both = jnp.where(left, a[i * W : (i + 1) * W], a[(i + 1) * W : (i + 2) * W])
                h = g * G + i
                att[b * W : (b + 1) * W, h * HW : (h + 2) * HW] = both.astype(BF)
    copies[1].wait()
    weight = recv[:, W : W + HW, :].reshape(HEADS * HW, TILE)
    stream = (dot(att[...], weight) + residual[...].astype(F32)).astype(BF)
    stream_out[...] = stream
    picked_out[...] = dot(pick[...], stream).astype(BF)


def lanes_at(index):
    return pl.ds(pl.multiple_of(index * TILE, TILE), TILE)


def row_scale(x):
    return lax.rsqrt(jnp.sum(x * x, axis=1, keepdims=True) / D + EPS)


def gated(scale, both):
    g = scale * both[:, :TILE]
    u = scale * both[:, TILE:]
    return (g / (1.0 + jnp.exp(-g)) * u).astype(BF)


def spread_kernel(meta, arrived, stream, out):
    for t in range(N_TP):
        r = jnp.where(meta[2] == G, t // G, t % G)
        out[t, :ROWS] = arrived[r]
        out[t, ROWS:] = stream[r]


def piece_copies(refs, lanes, target, sems):
    high, low = slice(0, HALF), slice(HALF, D)
    parts = [(i // 2, ref, low if i % 2 else high) for i, ref in enumerate(refs)]
    return [
        (s, pltpu.make_async_copy(ref.at[:, lanes], target(s, rows), sems.at[i]))
        for i, (s, ref, rows) in enumerate(parts)
    ]


def hidden_kernel(rows, *args):
    refs, (out, x, w, sems, row_sems) = args[: 2 * G], args[2 * G :]
    sets = [
        piece_copies(
            refs,
            slice(at, at + 2 * TILE),
            lambda s, r, j=j: w.at[j, s, r],
            sems.at[j],
        )
        for j, at in ((0, 0), (1, 3 * TILE))
    ]
    queue = [[c for step, c in sets[j] if step == s] for j in range(2) for s in range(G)]
    placed = [
        pltpu.make_async_copy(rows.at[t], x.at[:, pl.ds(t * TILE, TILE)], row_sems.at[t])
        for t in range(N_TP)
    ]
    for copy in placed:
        copy.start()
    for piece in queue[:AHEAD]:
        for copy in piece:
            copy.start()
    for copy in placed:
        copy.wait()
    for j, part in ((0, slice(0, ROWS)), (1, slice(ROWS, ALL_ROWS))):
        full = x[part, :]
        scale = row_scale(full.astype(F32))
        for s in range(G):
            at = j * G + s
            for copy in queue[at]:
                copy.wait()
            for piece in queue[at + AHEAD : at + AHEAD + 1]:
                for copy in piece:
                    copy.start()
            result = gated(scale, dot(full, w[j, s]))
            for k in range(G):
                out[k, part, s * TILE : (s + 1) * TILE] = result


def down_kernel(meta, hidden, *args):
    refs, (out, x, w, sems) = args[: 2 * G], args[2 * G :]
    sets = [
        piece_copies(
            refs,
            slice(at, at + TILE),
            lambda s, r, j=j: w.at[j, r, pl.ds(s * TILE, TILE)],
            sems.at[j],
        )
        for j, at in ((0, 2 * TILE), (1, 5 * TILE))
    ]
    for copies in sets:
        for _, copy in copies:
            copy.start()
    places = [lax.rem(meta[0] + (G - s), G) for s in range(G)]
    for s in range(G):
        for h in range(G):
            tile = places[s] * meta[2] + h * meta[3]
            x[:, lanes_at(tile)] = hidden[h, :, s * TILE : (s + 1) * TILE]
    for j, part in ((0, slice(0, ROWS)), (1, slice(ROWS, ALL_ROWS))):
        for _, copy in sets[j]:
            copy.wait()
        result = dot(x[part, :], w[j]).astype(BF)
        for s in range(G):
            out[places[s], part] = result[:, s * TILE : (s + 1) * TILE]


def return_kernel(parts, out):
    for r in range(G):
        out[r] = parts[r, :ROWS]


def combine_kernel(back, slots, weights_t, stream, parts, out):
    n = TOK_DEV
    own = jnp.concatenate([parts[r, ROWS:] for r in range(G)], axis=0)
    total = stream[...].astype(F32) + own.astype(F32)
    step = 256
    dims = (((0,), (0,)), ((), ()))
    for j in range(0, N_SP * CAP, step):
        place = lax.broadcasted_iota(jnp.int32, (step, n), 0) + j
        mix = jnp.where(place == slots[0:1, :], weights_t[0:1, :], 0.0) + jnp.where(
            place == slots[1:2, :], weights_t[1:2, :], 0.0
        )
        high = mix.astype(BF)
        low = (mix - high.astype(F32)).astype(BF)
        piece = back[j : j + step, :]
        total = total + dot(high, piece, dims) + dot(low, piece, dims)
    out[...] = total.astype(BF)


def layer(
    queries,
    keys_values,
    sink_logits,
    proj_weight,
    residual,
    norm_gain,
    routes,
    route_weights,
    gate_weight,
    up_weight,
    down_weight,
    shared_gate,
    shared_up,
    shared_down,
):
    sds = jax.ShapeDtypeStruct

    def kept(x):
        return pltpu.with_memory_space_constraint(x, pltpu.HBM)

    sp = lax.axis_index("sp")
    tp = lax.axis_index("tp")
    odd = lax.rem(sp, 2)
    high, low = tp // G, lax.rem(tp, G)
    r = jnp.where(odd == 0, high, low)
    h = jnp.where(odd == 0, low, high)
    meta = jnp.stack([r, h, jnp.where(odd == 0, G, 1), jnp.where(odd == 0, 1, G), sp]).astype(
        jnp.int32
    )

    payload = call(
        payload_kernel,
        sds((N_TP, WINDOW + HEAD_WIDTH + 16, TILE), BF),
        [SM, HB, HB],
        [
            pltpu.VMEM((HEAD_WIDTH, TOK_DEV), BF),
            pltpu.VMEM(proj_weight.shape, BF),
            pltpu.SemaphoreType.DMA((2,)),
        ],
    )(sink_logits, kept(queries.T), kept(proj_weight))
    recv = lax.all_to_all(payload, "tp", 0, 0, tiled=True)
    halo = lax.ppermute(
        keys_values[:, TOK_DEV - WINDOW :, :], "sp", [(i, i + 1) for i in range(N_SP - 1)]
    )

    half = sds((HALF, 6 * TILE), BF)
    own_top, own_bottom = call(
        prep_kernel,
        (half, half),
        [VM] + [HB] * 6,
        [
            pltpu.VMEM((4, D, TILE), BF),
            pltpu.VMEM((4, D, TILE), BF),
            pltpu.SemaphoreType.DMA((16,)),
        ],
        outs=(HB, HB),
    )(
        norm_gain.reshape(N_TP, TILE),
        kept(gate_weight[0]),
        kept(up_weight[0]),
        kept(down_weight[0]),
        kept(shared_gate),
        kept(shared_up),
        kept(shared_down),
    )
    behind_top = shifted(own_top, R_GROUPS, 1)
    ahead_bottom = shifted(own_bottom, R_GROUPS, 3)
    behind_bottom = shifted(own_bottom, R_GROUPS, 1)
    ahead_top = shifted(own_top, R_GROUPS, 3)
    top = shifted(behind_top, R_GROUPS, 1)
    bottom = shifted(ahead_bottom, R_GROUPS, 3)
    weights = (
        own_top, own_bottom, behind_top, behind_bottom, top, bottom, ahead_top, ahead_bottom
    )

    rows = N_SP * CAP
    stream, picked, slots = call(
        front_kernel,
        (sds((TOK_DEV, TILE), BF), sds((rows, TILE), BF), sds((2, TOK_DEV), jnp.int32)),
        [SM, VM, HB, VM, HB, HB],
        [
            pltpu.VMEM(recv.shape, BF),
            pltpu.VMEM(keys_values.shape, BF),
            pltpu.VMEM(residual.shape, BF),
            pltpu.VMEM((rows, TOK_DEV), BF),
            pltpu.VMEM((TOK_DEV, HEADS * HEAD_WIDTH), BF),
            pltpu.SemaphoreType.DMA((6,)),
        ],
    )(meta, routes.T, kept(recv), halo, kept(keys_values), kept(residual))

    arrived = lax.all_to_all(picked.reshape(N_SP, CAP, TILE), "sp", 0, 0, tiled=True)

    sent = call(
        spread_kernel,
        sds((N_TP, ALL_ROWS, TILE), BF),
        [SM, VM, VM],
    )(meta, arrived.reshape(G, ROWS, TILE), stream.reshape(G, OWN, TILE))
    rows = lax.all_to_all(sent, "tp", 0, 0, tiled=True)

    hidden = call(
        hidden_kernel,
        sds((G, ALL_ROWS, G * TILE), BF),
        [HB] + [HB] * (2 * G),
        [
            pltpu.VMEM((ALL_ROWS, D), BF),
            pltpu.VMEM((2, G, D, 2 * TILE), BF),
            pltpu.SemaphoreType.DMA((2, 2 * G)),
            pltpu.SemaphoreType.DMA((N_TP,)),
        ],
    )(rows, *weights)
    hidden = swapped(hidden, H_GROUPS)

    parts = call(
        down_kernel,
        sds((G, ALL_ROWS, TILE), BF),
        [SM, VM] + [HB] * (2 * G),
        [
            pltpu.VMEM((ALL_ROWS, D), BF),
            pltpu.VMEM((2, D, G * TILE), BF),
            pltpu.SemaphoreType.DMA((2, 2 * G)),
        ],
    )(meta, hidden, *weights)
    parts = swapped(parts, R_GROUPS)

    outgoing = call(return_kernel, sds((G, ROWS, TILE), BF), [VM])(parts)
    back = lax.all_to_all(outgoing.reshape(N_SP, CAP, TILE), "sp", 0, 0, tiled=True)
    return call(combine_kernel, sds((TOK_DEV, TILE), BF), [VM, VM, VM, VM, VM])(
        back.reshape(N_SP * CAP, TILE), slots, route_weights.T, stream, parts
    )


def solution(mesh):
    placed = (
        P("sp", "tp"),
        P(None, "sp", None),
        P("tp"),
        P("tp", None),
        P("sp", "tp"),
        P(),
        P("sp", None),
        P("sp", None),
        P("sp", None, "tp"),
        P("sp", None, "tp"),
        P("sp", None, "tp"),
        P(None, "tp"),
        P(None, "tp"),
        P(None, "tp"),
    )
    return jax.shard_map(
        layer, mesh=mesh, in_specs=placed, out_specs=P("sp", "tp"), check_vma=False
    )
```
